128 devices in a mesh: kv: 16 (over z, x), tp: 8 (over y, core).
Axes of the slice: x: 4, y: 4, z: 4, core: 2. Of those that a mesh axis runs over, the one named last changes fastest.
Arguments:
- tokens: bfloat16 [128, 4096], P('tp', 'kv'), may hold values from -16 to 16
- cache_keys: bfloat16 [128, 16384, 2, 128], P('tp', 'kv'), may hold values from -512 to 512
- cache_values: bfloat16 [128, 16384, 2, 128], P('tp', 'kv'), may hold values from -6 to 6
- attn_gain: float32 [4096], P('kv'), may hold values from 0.1 to 1.9
- w_query: bfloat16 [4096, 2048], P('kv'), may hold values from -0.15625 to 0.15625
- w_key: bfloat16 [4096, 256], P('kv'), may hold values from -0.09375 to 0.09375
- w_value: bfloat16 [4096, 256], P('kv'), may hold values from -0.09375 to 0.09375
- lambdas: float32 [16], replicated, may hold values from 0.3 to 0.8
- head_gain: float32 [128], replicated, may hold values from 0.1 to 1.9
- w_out: bfloat16 [2048, 4096], P(None, 'kv'), may hold values from -0.125 to 0.125
- mlp_gain: float32 [4096], P('kv'), may hold values from 0.1 to 1.9
- w_up: bfloat16 [4096, 16384], P('kv', 'tp'), may hold values from -0.09375 to 0.09375
- w_down: bfloat16 [16384, 4096], P('tp', 'kv'), may hold values from -0.046875 to 0.046875
Outputs:
- mixed: bfloat16 [128, 4096], P('tp', 'kv')
- new_keys: bfloat16 [128, 2, 128], P('tp')
- new_values: bfloat16 [128, 2, 128], P('tp')
The draws below stay inside these ranges and needn't reach their ends.
All inputs are finite; a program needn't handle non-finite values.
Results may differ from the reference program's by a relative error of at most 0.014.
Values may be sent and summed in bfloat16 or wider, within the bound.
No kernel may reach another device: no remote copies, remote signals or barrier semaphores. Data moves between devices by JAX's collectives and lax.ppermute only.
A program may use at most 128 MiB of HBM per device.

```python
import jax
import jax.numpy as jnp
from jax import lax

D = 4096
HEADS = 16
KV_HEADS = 2
QK = 64
VD = 128
FF = 16384
BATCH = 128
CTX_DEV = 1024
CTX = 16384
N_KV = 16
N_TP = 8


def draw_tokens(key, part):
    key_scale, key_base = jax.random.split(jax.random.fold_in(key, 11))
    col_scales = jnp.exp(jax.random.uniform(key_scale, (D // 128,), jnp.float32, -1.2, 1.2))
    columns = jnp.repeat(col_scales, 128)
    base_vals = jax.random.normal(key_base, (BATCH, D), jnp.float32)
    return jnp.clip(base_vals * columns[None, :], -16.0, 16.0).astype(jnp.bfloat16)


def draw_cache_keys(key, part):
    key_base, key_mark = jax.random.split(jax.random.fold_in(key, 23))
    base_vals = jax.random.normal(key_base, (BATCH, CTX, KV_HEADS, 2 * QK), jnp.float32)
    return jnp.clip(base_vals, -512.0, 512.0).astype(jnp.bfloat16)


def steps_of(stream_key, shape, pieces, least, largest):
    factor_of = 1.0
    for position, blocks in pieces:
        heights = jax.random.uniform(jax.random.fold_in(jax.random.fold_in(stream_key, 6), position), (blocks,), jnp.float32, least / len(pieces), largest / len(pieces))
        factor_of = factor_of * jnp.repeat(jnp.exp(heights), shape[position] // blocks).reshape((-1,) + (1,) * (len(shape) - 1 - position))
    return factor_of


def normal_values(stream_key, extent, spread, bound, pieces=(), held_as=jnp.bfloat16):
    gain = steps_of(stream_key, extent, pieces, -0.22, 0.18) if pieces else 1.0
    values = jax.random.normal(stream_key, extent, jnp.float32) * spread * gain
    return jnp.minimum(jnp.maximum(values, -bound), bound).astype(held_as)


def setup_inputs(seed: int = 0) -> dict:
    splits = jax.random.split(jax.random.key(seed), 14)
    tokens = draw_tokens(jax.random.fold_in(splits[13], 71), 0)
    cache_keys = draw_cache_keys(jax.random.fold_in(splits[13], 71), 0)
    cache_values = normal_values(splits[2], (BATCH, CTX, KV_HEADS, VD), 1.0, 6.0, ((0, 8), (1, 16)))
    attn_gain = jnp.clip(1.0 + 0.18 * jax.random.normal(splits[3], (D,), jnp.float32), 0.1, 1.9)
    w_query = normal_values(splits[4], (D, HEADS * 2 * QK), (D // 3) ** -0.5, 0.15625, ((0, 16),))
    w_key = normal_values(splits[5], (D, KV_HEADS * 2 * QK), D ** -0.5, 0.09375, ((0, 16),))
    w_value = normal_values(splits[6], (D, KV_HEADS * VD), D ** -0.5, 0.09375, ((0, 16),))
    lambdas = jnp.clip(jax.random.uniform(splits[7], (HEADS,), jnp.float32, 0.3, 0.8), 0.3, 0.8)
    head_gain = jnp.clip(1.0 + 0.18 * jax.random.normal(splits[8], (VD,), jnp.float32), 0.1, 1.9)
    w_out = normal_values(splits[9], (HEADS * VD, D), (HEADS * VD) ** -0.5, 0.125, ((1, 16),))
    mlp_gain = jnp.clip(1.0 + 0.18 * jax.random.normal(splits[10], (D,), jnp.float32), 0.1, 1.9)
    w_up = normal_values(splits[11], (D, FF), D ** -0.5, 0.09375, ((0, 16), (1, 8)))
    w_down = normal_values(splits[12], (FF, D), FF ** -0.5, 0.046875, ((0, 8), (1, 16)))
    return dict(tokens=tokens, cache_keys=cache_keys, cache_values=cache_values, attn_gain=attn_gain, w_query=w_query, w_key=w_key, w_value=w_value, lambdas=lambdas, head_gain=head_gain, w_out=w_out, mlp_gain=mlp_gain, w_up=w_up, w_down=w_down)


norm_eps = 1e-06

def reference(tokens, cache_keys, cache_values, attn_gain, w_query, w_key, w_value, lambdas, head_gain, w_out, mlp_gain, w_up, w_down):
    tok_f = tokens.astype(jnp.float32)
    inv_one = lax.rsqrt(lax.optimization_barrier(jnp.mean(tok_f * tok_f, axis=1, keepdims=True)) + norm_eps)
    scaled = (tok_f * attn_gain[None, :]).astype(jnp.bfloat16)
    query = (jnp.dot(scaled, w_query, preferred_element_type=jnp.float32) * inv_one).astype(jnp.bfloat16)
    new_keys = (jnp.dot(scaled, w_key, preferred_element_type=jnp.float32) * inv_one).astype(jnp.bfloat16)
    new_values = (jnp.dot(scaled, w_value, preferred_element_type=jnp.float32) * inv_one).astype(jnp.bfloat16)
    head_group = HEADS // KV_HEADS
    query_five = query.reshape(BATCH, KV_HEADS, head_group, 2, QK).astype(jnp.float32)

    def one_block(index):
        begin = index * CTX_DEV
        keys_blk = lax.dynamic_slice_in_dim(cache_keys, begin, CTX_DEV, 1)
        keys_blk = keys_blk.reshape(BATCH, CTX_DEV, KV_HEADS, 2, QK).astype(jnp.float32)
        vals_blk = lax.dynamic_slice_in_dim(cache_values, begin, CTX_DEV, 1).astype(jnp.float32)
        scores = jnp.einsum('bkgcd,bpkcd->bkgcp', query_five, keys_blk) * QK ** (-0.5)
        block_top = lax.optimization_barrier(jnp.max(scores, axis=-1))
        exp_scores = jnp.exp(scores - block_top[..., None])
        block_total = lax.optimization_barrier(jnp.sum(exp_scores, axis=-1))
        weights = exp_scores.astype(jnp.bfloat16).astype(jnp.float32)
        block_acc = jnp.einsum('bkgcp,bpke->bkgce', weights, vals_blk)
        return (block_top, block_total, block_acc)
    tops, totals, accs = lax.map(one_block, jnp.arange(N_KV, dtype=jnp.int32))
    peak = lax.optimization_barrier(jnp.max(tops, axis=0))
    factor = jnp.exp(tops - peak[None])
    total = lax.optimization_barrier(jnp.sum(totals * factor, axis=0))
    acc = lax.optimization_barrier(jnp.sum(accs * factor[..., None], axis=0))
    lam_heads = lambdas.reshape(KV_HEADS, head_group)[None, :, :, None]
    head_out = acc[:, :, :, 0] / total[:, :, :, 0, None] - lam_heads * acc[:, :, :, 1] / total[:, :, :, 1, None]
    mean_sq = lax.optimization_barrier(jnp.mean(head_out * head_out, axis=-1, keepdims=True))
    normed = head_out * lax.rsqrt(mean_sq + 1.0 / CTX) * head_gain
    normed = normed.astype(jnp.bfloat16).reshape(BATCH, HEADS * VD)
    residual = (tok_f + jnp.dot(normed, w_out, preferred_element_type=jnp.float32)).astype(jnp.bfloat16)
    res_f = residual.astype(jnp.float32)
    inv_two = lax.rsqrt(lax.optimization_barrier(jnp.mean(res_f * res_f, axis=1, keepdims=True)) + norm_eps)
    gained = (res_f * mlp_gain[None, :]).astype(jnp.bfloat16)
    pre_act = jnp.dot(gained, w_up, preferred_element_type=jnp.float32) * inv_two
    act_rows = jnp.square(jax.nn.relu(pre_act)).astype(jnp.bfloat16)
    act_blocks = act_rows.reshape(BATCH, N_TP, FF // N_TP).astype(jnp.float32)
    down_blocks = w_down.reshape(N_TP, FF // N_TP, D).astype(jnp.float32)
    parts = jnp.einsum('btf,tfd->tbd', act_blocks, down_blocks)
    rounded = lax.optimization_barrier(parts.astype(jnp.bfloat16)).astype(jnp.float32)
    ffn_out = lax.optimization_barrier(jnp.sum(rounded, axis=0))
    mixed = (res_f + ffn_out).astype(jnp.bfloat16)
    return (mixed, new_keys.reshape(BATCH, KV_HEADS, 2 * QK), new_values.reshape(BATCH, KV_HEADS, VD))
```

```python
import functools

import jax
import jax.numpy as jnp
from jax import lax
from jax.experimental import pallas as pl
from jax.experimental.pallas import tpu as pltpu
from jax.sharding import Mesh
from jax.sharding import PartitionSpec as P

KV = ("z", "x")
TP = ("y", "c")
EPS = 1e-06
LANES = 128
F32 = jnp.float32
BF16 = jnp.bfloat16
VMEM = pl.BlockSpec(memory_space=pltpu.VMEM)
HBM = pl.BlockSpec(memory_space=pltpu.HBM)


def local_call(body, name, outs, *args, flops=0, scratch=(), limit=8, far=()):
    cost = pl.CostEstimate(
        flops=flops,
        bytes_accessed=sum(a.size * a.dtype.itemsize for a in args),
        transcendentals=0,
    )
    return pl.pallas_call(
        body,
        name=name,
        out_shape=outs,
        in_specs=[HBM if i in far else VMEM for i in range(len(args))],
        out_specs=jax.tree.map(lambda _: VMEM, outs),
        scratch_shapes=list(scratch),
        cost_estimate=cost,
        compiler_params=pltpu.CompilerParams(vmem_limit_bytes=int(limit * 2**20)),
    )(*args)


def from_peers(shard, axis):
    peers = lax.axis_size(axis)
    return [
        lax.ppermute(shard, axis, [(i, i ^ k) for i in range(peers)])
        for k in range(1, peers)
    ]


def exchanged(tiles, axis):
    return lax.all_to_all(tiles, axis, 0, 0, tiled=True)


def dot(a, b, contract=((1,), (0,))):
    return lax.dot_general(a, b, (contract, ((), ())), preferred_element_type=F32)


def pieces(x):
    hi = x.astype(BF16).astype(F32)
    mid = (x - hi).astype(BF16).astype(F32)
    lo = (x - hi - mid).astype(BF16).astype(F32)
    return hi, mid, lo


def query_body(scaled_ref, squares_ref, w_ref, q_ref):
    q = dot(scaled_ref[...], w_ref[...])
    tiles = q_ref.shape[0] - 1
    for h in range(tiles):
        q_ref[h] = q[:, h * LANES : (h + 1) * LANES]
    q_ref[tiles] = squares_ref[...]


def new_kv_body(scaled_ref, wk_ref, wv_ref, kv_ref):
    rows = scaled_ref.shape[0]
    at = 0
    for w in (wk_ref, wv_ref):
        part = dot(scaled_ref[...], w[...]).astype(BF16)
        for t in range(part.shape[1] // LANES):
            kv_ref[at : at + rows] = part[:, t * LANES : (t + 1) * LANES]
            at += rows


def attention_body(width, q0, q1, q2, q3, kv_ref, k_ref, v_ref, out_ref, inv_ref, q_scr):
    rows, spots, _ = k_ref.shape
    heads = q0.shape[0] - 1
    total_q = (q0[...] + q1[...]) + (q2[...] + q3[...])
    inv = lax.rsqrt(total_q[heads] / width + EPS)
    inv_ref[...] = inv
    for h in range(heads):
        q_scr[:, h, :] = (total_q[h] * inv).astype(BF16).astype(F32) * 0.125
    vecs = 2 * heads
    lane = lax.broadcasted_iota(jnp.int32, (vecs, LANES), 1)
    row = lax.broadcasted_iota(jnp.int32, (vecs, LANES), 0)
    own_half = (lane // 64) == (row // heads)
    wide_lane = lax.broadcasted_iota(jnp.int32, (vecs, spots), 1)
    wide_row = lax.broadcasted_iota(jnp.int32, (vecs, spots), 0)
    own_head = (wide_lane % 2) == ((wide_row % heads) // (heads // 2))

    def step(b, stats):
        q16 = q_scr[b]
        both = jnp.concatenate([q16, q16], axis=0)
        q32 = jnp.where(own_half, both, 0.0).astype(BF16)
        s = dot(q32, k_ref[b], ((1,), (1,)))
        s = jnp.where(own_head, s, -1e30)
        top = jnp.max(s, axis=1, keepdims=True)
        e = jnp.exp(s - top)
        total = jnp.sum(e, axis=1, keepdims=True)
        acc = dot(e.astype(BF16), v_ref[b])
        out_ref[pl.ds(pl.multiple_of(b * vecs, vecs), vecs), :] = acc.astype(BF16)
        here = (lane % 16) == b
        return jnp.where(
            here & (lane < 48), top, jnp.where(here & (lane < 96), total, stats)
        )

    stats = lax.fori_loop(0, rows, step, jnp.zeros((vecs, LANES), F32), unroll=2)
    hi, mid, lo = pieces(stats)
    kind = (lane // 16) % 3
    at = rows * vecs
    out_ref[at : at + vecs] = jnp.where(
        kind == 0, hi, jnp.where(kind == 1, mid, lo)
    ).astype(BF16)
    out_ref[at + vecs :] = kv_ref[...]


def opened_stats(ref, at, vecs):
    p = ref[at : at + vecs].astype(F32)
    whole = p + pltpu.roll(p, LANES - 16, 1) + pltpu.roll(p, LANES - 32, 1)
    return whole, pltpu.roll(whole, LANES - 48, 1)


def merged_stats(refs, at, vecs):
    opened = [opened_stats(r, at, vecs) for r in refs]
    tops = [o[0] for o in opened]
    peak = jnp.maximum(jnp.maximum(tops[0], tops[1]), jnp.maximum(tops[2], tops[3]))
    factors = [jnp.exp(t - peak) for t in tops]
    parts = [f * o[1] for f, o in zip(factors, opened)]
    total = (parts[0] + parts[1]) + (parts[2] + parts[3])
    return peak, total, factors


def weighted(refs, weights, b, start, count, weight_row):
    parts = []
    for r, w in zip(refs, weights):
        block = r[start : start + count].astype(F32)
        parts.append(block * w[weight_row : weight_row + count, b : b + 1])
    return (parts[0] + parts[1]) + (parts[2] + parts[3])


def merge_body(rows, vecs, p0, p1, p2, p3, out_ref):
    refs = (p0, p1, p2, p3)
    at = rows * vecs
    peak, total, factors = merged_stats(refs, at, vecs)
    for b in range(rows):
        acc = weighted(refs, factors, b, b * vecs, vecs, 0)
        out_ref[b * vecs : (b + 1) * vecs] = acc.astype(BF16)
    lane = lax.broadcasted_iota(jnp.int32, (vecs, LANES), 1)
    both = jnp.where(lane < 16, peak, 0.0)
    both = both + pltpu.roll(both, 16, 1) + pltpu.roll(both, 32, 1)
    tot = jnp.where(lane < 16, total, 0.0)
    tot = pltpu.roll(tot, 48, 1) + pltpu.roll(tot, 64, 1) + pltpu.roll(tot, 80, 1)
    hi, mid, lo = pieces(both + tot)
    kind = (lane // 16) % 3
    out_ref[at : at + vecs] = jnp.where(
        kind == 0, hi, jnp.where(kind == 1, mid, lo)
    ).astype(BF16)
    rest = at + vecs
    a, b_, c, d = [r[rest:].astype(F32) for r in refs]
    out_ref[rest:] = ((a + b_) + (c + d)).astype(BF16)


def residual_body(
    rows, vecs, ctx, p0, p1, p2, p3, inv_ref, lam_ref, gain_ref, tok_ref, w_ref,
    res_ref, all_ref, nk_ref, nv_ref, n_scr,
):
    refs = (p0, p1, p2, p3)
    heads = vecs // 2
    at = rows * vecs
    _, total, factors = merged_stats(refs, at, vecs)
    lane = lax.broadcasted_iota(jnp.int32, (vecs, LANES), 1)
    scale = 1.0 / jnp.where(lane < 16, total, 1.0)
    lam = lam_ref[...]
    weights = [
        jnp.concatenate([(f * scale)[:heads], (f * scale)[heads:] * lam], axis=0)
        for f in factors
    ]
    gain = gain_ref[...]
    for b in range(rows):
        first = weighted(refs, weights, b, b * vecs, heads, 0)
        second = weighted(refs, weights, b, b * vecs + heads, heads, heads)
        out = first - second
        mean_sq = jnp.mean(out * out, axis=1, keepdims=True)
        n_scr[:, b, :] = out * lax.rsqrt(mean_sq + 1.0 / ctx) * gain
    normed = jnp.concatenate([n_scr[h].astype(BF16) for h in range(heads)], axis=1)
    res = (tok_ref[...].astype(F32) + dot(normed, w_ref[...])).astype(BF16)
    res_ref[...] = res
    for t in range(all_ref.shape[0]):
        all_ref[t] = res
    rest = at + vecs
    a, b_, c, d = [r[rest:].astype(F32) for r in refs]
    kv = (a + b_) + (c + d)
    inv = inv_ref[...]
    for t in range(2):
        nk_ref[:, t, :] = (kv[t * rows : (t + 1) * rows] * inv).astype(BF16)
        nv_ref[:, t, :] = (kv[(2 + t) * rows : (3 + t) * rows] * inv).astype(BF16)


def diagonal(size):
    a = lax.broadcasted_iota(jnp.int32, (size, size), 0)
    return a == lax.broadcasted_iota(jnp.int32, (size, size), 1)


def up_body(res_ref, gain_ref, w_ref, out_ref):
    groups, rows, width = res_ref.shape
    batch = groups * rows
    res = res_ref[...].reshape(batch, width).astype(F32)
    gained = (res * gain_ref[...]).astype(BF16)
    squares = jnp.sum(res * res, axis=1, keepdims=True)
    line = jnp.sum(jnp.where(diagonal(batch), squares, 0.0), axis=0, keepdims=True)
    hi, mid, lo = pieces(jnp.broadcast_to(line, (16, batch)))
    sub = lax.broadcasted_iota(jnp.int32, (16, batch), 0)
    tail = jnp.where(sub == 0, hi, jnp.where(sub == 1, mid, jnp.where(sub == 2, lo, 0.0)))
    tail = tail.astype(BF16)
    up = dot(gained, w_ref[...])
    for d in range(out_ref.shape[0]):
        out_ref[d, :batch] = up[:, d * LANES : (d + 1) * LANES].astype(BF16)
        out_ref[d, batch:] = tail


def act_body(width, in_ref, out_ref):
    peers, batch, _ = out_ref.shape
    up = in_ref[0, :batch].astype(F32)
    tail = in_ref[0, batch:].astype(F32)
    for p in range(1, peers):
        up = up + in_ref[p, :batch].astype(F32)
        tail = tail + in_ref[p, batch:].astype(F32)
    line = jnp.sum(tail, axis=0, keepdims=True)
    squares = jnp.sum(jnp.where(diagonal(batch), line, 0.0), axis=1, keepdims=True)
    pre = up * lax.rsqrt(squares / width + EPS)
    act = jnp.square(jnp.maximum(pre, 0.0)).astype(BF16)
    for p in range(peers):
        out_ref[p] = act


def down_body(act_ref, w_ref, out_ref):
    peers = act_ref.shape[0]
    acts = jnp.concatenate([act_ref[p] for p in range(peers)], axis=1)
    down = dot(acts, w_ref[...]).astype(BF16)
    out_ref[...] = down.reshape(out_ref.shape)


def final_body(down_ref, res_ref, out_ref):
    total = down_ref[0].astype(F32)
    for t in range(1, down_ref.shape[0]):
        total = total + down_ref[t].astype(F32)
    out_ref[...] = (res_ref[...].astype(F32) + total).astype(BF16)


def shards(
    tokens,
    cache_keys,
    cache_values,
    attn_gain,
    w_query,
    w_key,
    w_value,
    lambdas,
    head_gain,
    w_out,
    mlp_gain,
    w_up,
    w_down,
):
    rows, tok_width = tokens.shape
    n_kv = lax.axis_size(KV)
    n_tp = lax.axis_size(TP)
    width = tok_width * n_kv
    heads = lambdas.shape[0]
    ctx_local, kv_heads, _ = cache_keys.shape[1:]
    ctx = ctx_local * n_kv
    spots = ctx_local * kv_heads
    vecs = 2 * heads
    struct = jax.ShapeDtypeStruct
    batch = rows * n_tp

    tok = tokens.astype(F32)
    scaled = (tok * attn_gain[None, :]).astype(BF16)
    squares = jnp.sum(tok * tok, axis=1, keepdims=True)
    q_part = local_call(
        query_body,
        "query",
        struct((heads + 1, rows, LANES), F32),
        scaled,
        jnp.broadcast_to(squares, (rows, LANES)),
        w_query,
        flops=2 * rows * tok_width * w_query.shape[1],
    )
    kv_part = local_call(
        new_kv_body,
        "new_kv",
        struct((4 * rows, LANES), BF16),
        scaled,
        w_key,
        w_value,
        flops=1 << 33,
    )
    a, b, c = from_peers(q_part, "x")
    q_half = (q_part + a) + (b + c)
    a, b, c = from_peers(q_half, "z")
    packed = rows * vecs + vecs + 4 * rows
    payload, inv_one = local_call(
        functools.partial(attention_body, float(width)),
        "attention",
        (struct((packed, LANES), BF16), struct((rows, LANES), F32)),
        q_half,
        a,
        b,
        c,
        kv_part,
        cache_keys.reshape(rows, spots, LANES),
        cache_values.reshape(rows, spots, LANES),
        flops=4 * rows * vecs * spots * LANES,
        limit=24,
        scratch=(pltpu.VMEM((rows, heads, LANES), F32),),
    )
    payload = local_call(
        functools.partial(merge_body, rows, vecs),
        "merge",
        struct((packed, LANES), BF16),
        payload,
        *from_peers(payload, "x"),
        flops=packed * LANES * 8,
    )
    residual, to_all, new_keys, new_values = local_call(
        functools.partial(residual_body, rows, vecs, float(ctx)),
        "residual",
        (
            struct((rows, tok_width), BF16),
            struct((n_tp, rows, tok_width), BF16),
            struct((rows, kv_heads, LANES), BF16),
            struct((rows, kv_heads, LANES), BF16),
        ),
        payload,
        *from_peers(payload, "z"),
        inv_one,
        jnp.broadcast_to(lambdas[:, None], (heads, LANES)),
        head_gain[None, :],
        tokens,
        w_out,
        flops=2 * rows * heads * LANES * tok_width,
        scratch=(pltpu.VMEM((heads, rows, LANES), F32),),
    )
    everyone = exchanged(to_all, TP)
    up = local_call(
        up_body,
        "up",
        struct((n_kv, batch + 16, LANES), BF16),
        everyone,
        mlp_gain[None, :],
        w_up,
        flops=2 * batch * tok_width * n_kv * LANES,
    )
    acts = local_call(
        functools.partial(act_body, float(width)),
        "act",
        struct((n_kv, batch, LANES), BF16),
        exchanged(up, KV),
        flops=batch * LANES * 40,
    )
    down = local_call(
        down_body,
        "down",
        struct((n_tp, rows, tok_width), BF16),
        exchanged(acts, KV),
        w_down,
        flops=2 * batch * tok_width * n_kv * LANES,
    )
    mixed = local_call(
        final_body,
        "final",
        struct((rows, tok_width), BF16),
        exchanged(down, TP),
        residual,
        flops=rows * tok_width * 10,
    )
    return mixed, new_keys, new_values


def solution(mesh):
    split = Mesh(mesh.devices.reshape(4, 4, 4, 2), ("z", "x", "y", "c"))
    placed = (
        P(TP, KV),
        P(TP, KV, None, None),
        P(TP, KV, None, None),
        P(KV),
        P(KV, None),
        P(KV, None),
        P(KV, None),
        P(),
        P(),
        P(None, KV),
        P(KV),
        P(KV, TP),
        P(TP, KV),
    )
    return jax.shard_map(
        shards,
        mesh=split,
        in_specs=placed,
        out_specs=(P(TP, KV), P(TP, None, None), P(TP, None, None)),
        check_vma=False,
    )
```

```python
import functools

import jax
import jax.numpy as jnp
from jax import lax
from jax.experimental import pallas as pl
from jax.experimental.pallas import tpu as pltpu
from jax.sharding import Mesh
from jax.sharding import PartitionSpec as P

KV = ("z", "x")
TP = ("y", "c")
EPS = 1e-06
LANES = 128
F32 = jnp.float32
BF16 = jnp.bfloat16
VMEM = pl.BlockSpec(memory_space=pltpu.VMEM)
HBM = pl.BlockSpec(memory_space=pltpu.HBM)


def local_call(body, name, outs, *args, flops=0, scratch=(), limit=8, far=()):
    cost = pl.CostEstimate(
        flops=flops,
        bytes_accessed=sum(a.size * a.dtype.itemsize for a in args),
        transcendentals=0,
    )
    return pl.pallas_call(
        body,
        name=name,
        out_shape=outs,
        in_specs=[HBM if i in far else VMEM for i in range(len(args))],
        out_specs=jax.tree.map(lambda _: VMEM, outs),
        scratch_shapes=list(scratch),
        cost_estimate=cost,
        compiler_params=pltpu.CompilerParams(vmem_limit_bytes=int(limit * 2**20)),
    )(*args)


def from_peers(shard, axis):
    peers = lax.axis_size(axis)
    return [
        lax.ppermute(shard, axis, [(i, i ^ k) for i in range(peers)])
        for k in range(1, peers)
    ]


def exchanged(tiles, axis):
    return lax.all_to_all(tiles, axis, 0, 0, tiled=True)


def dot(a, b, contract=((1,), (0,))):
    return lax.dot_general(a, b, (contract, ((), ())), preferred_element_type=F32)


def pieces(x):
    hi = x.astype(BF16).astype(F32)
    mid = (x - hi).astype(BF16).astype(F32)
    lo = (x - hi - mid).astype(BF16).astype(F32)
    return hi, mid, lo


def query_body(scaled_ref, squares_ref, w_ref, q_ref):
    q = dot(scaled_ref[...], w_ref[...])
    tiles = q_ref.shape[0] - 1
    for h in range(tiles):
        q_ref[h] = q[:, h * LANES : (h + 1) * LANES]
    q_ref[tiles] = squares_ref[...]


def new_kv_body(scaled_ref, wk_ref, wv_ref, kv_ref):
    rows = scaled_ref.shape[0]
    at = 0
    for w in (wk_ref, wv_ref):
        part = dot(scaled_ref[...], w[...]).astype(BF16)
        for t in range(part.shape[1] // LANES):
            kv_ref[at : at + rows] = part[:, t * LANES : (t + 1) * LANES]
            at += rows


def attention_body(width, q0, q1, q2, q3, kv_ref, k_ref, v_ref, out_ref, inv_ref, q_scr, s_scr):
    rows, spots, _ = k_ref.shape
    heads = q0.shape[0] - 1
    total_q = (q0[...] + q1[...]) + (q2[...] + q3[...])
    inv = lax.rsqrt(total_q[heads] / width + EPS)
    inv_ref[...] = inv
    for h in range(heads):
        q_scr[:, h, :] = (total_q[h] * inv).astype(BF16).astype(F32) * 0.125
    vecs = 2 * heads
    lane = lax.broadcasted_iota(jnp.int32, (vecs, LANES), 1)
    row = lax.broadcasted_iota(jnp.int32, (vecs, LANES), 0)
    own_half = (lane // 64) == (row // heads)
    wide_lane = lax.broadcasted_iota(jnp.int32, (vecs, spots), 1)
    wide_row = lax.broadcasted_iota(jnp.int32, (vecs, spots), 0)
    own_head = (wide_lane % 2) == ((wide_row % heads) // (heads // 2))

    def scores(b):
        q16 = q_scr[b]
        both = jnp.concatenate([q16, q16], axis=0)
        q32 = jnp.where(own_half, both, 0.0).astype(BF16)
        return dot(q32, k_ref[b], ((1,), (1,)))

    def finish(b, s, stats):
        s = jnp.where(own_head, s, -1e30)
        top = jnp.max(s, axis=1, keepdims=True)
        e = jnp.exp(s - top)
        total = jnp.sum(e, axis=1, keepdims=True)
        acc = dot(e.astype(BF16), v_ref[b])
        out_ref[pl.ds(pl.multiple_of(b * vecs, vecs), vecs), :] = acc.astype(BF16)
        here = (lane % 16) == b
        return jnp.where(
            here & (lane < 48), top, jnp.where(here & (lane < 96), total, stats)
        )

    deep = 4
    s_scr[0] = scores(0)

    def step(i, stats):
        for u in range(deep):
            b = i * deep + u
            current = s_scr[u % 2]
            following = scores(jnp.minimum(b + 1, rows - 1))
            stats = finish(b, current, stats)
            s_scr[(u + 1) % 2] = following
        return stats

    stats = lax.fori_loop(0, rows // deep, step, jnp.zeros((vecs, LANES), F32))
    hi, mid, lo = pieces(stats)
    kind = (lane // 16) % 3
    at = rows * vecs
    out_ref[at : at + vecs] = jnp.where(
        kind == 0, hi, jnp.where(kind == 1, mid, lo)
    ).astype(BF16)
    out_ref[at + vecs :] = kv_ref[...]


def opened_stats(ref, at, vecs):
    p = ref[at : at + vecs].astype(F32)
    whole = p + pltpu.roll(p, LANES - 16, 1) + pltpu.roll(p, LANES - 32, 1)
    return whole, pltpu.roll(whole, LANES - 48, 1)


def merged_stats(refs, at, vecs):
    opened = [opened_stats(r, at, vecs) for r in refs]
    tops = [o[0] for o in opened]
    peak = jnp.maximum(jnp.maximum(tops[0], tops[1]), jnp.maximum(tops[2], tops[3]))
    factors = [jnp.exp(t - peak) for t in tops]
    parts = [f * o[1] for f, o in zip(factors, opened)]
    total = (parts[0] + parts[1]) + (parts[2] + parts[3])
    return peak, total, factors


def weighted(refs, weights, b, start, count, weight_row):
    parts = []
    for r, w in zip(refs, weights):
        block = r[start : start + count].astype(F32)
        parts.append(block * w[weight_row : weight_row + count, b : b + 1])
    return (parts[0] + parts[1]) + (parts[2] + parts[3])


def merge_body(rows, vecs, p0, p1, p2, p3, out_ref):
    refs = (p0, p1, p2, p3)
    at = rows * vecs
    peak, total, factors = merged_stats(refs, at, vecs)
    for b in range(rows):
        acc = weighted(refs, factors, b, b * vecs, vecs, 0)
        out_ref[b * vecs : (b + 1) * vecs] = acc.astype(BF16)
    lane = lax.broadcasted_iota(jnp.int32, (vecs, LANES), 1)
    both = jnp.where(lane < 16, peak, 0.0)
    both = both + pltpu.roll(both, 16, 1) + pltpu.roll(both, 32, 1)
    tot = jnp.where(lane < 16, total, 0.0)
    tot = pltpu.roll(tot, 48, 1) + pltpu.roll(tot, 64, 1) + pltpu.roll(tot, 80, 1)
    hi, mid, lo = pieces(both + tot)
    kind = (lane // 16) % 3
    out_ref[at : at + vecs] = jnp.where(
        kind == 0, hi, jnp.where(kind == 1, mid, lo)
    ).astype(BF16)
    rest = at + vecs
    a, b_, c, d = [r[rest:].astype(F32) for r in refs]
    out_ref[rest:] = ((a + b_) + (c + d)).astype(BF16)


def residual_body(
    rows, vecs, ctx, p0, p1, p2, p3, inv_ref, lam_ref, gain_ref, tok_ref, w_ref,
    res_ref, all_ref, nk_ref, nv_ref, n_scr,
):
    refs = (p0, p1, p2, p3)
    heads = vecs // 2
    at = rows * vecs
    _, total, factors = merged_stats(refs, at, vecs)
    lane = lax.broadcasted_iota(jnp.int32, (vecs, LANES), 1)
    scale = 1.0 / jnp.where(lane < 16, total, 1.0)
    lam = lam_ref[...]
    weights = [
        jnp.concatenate([(f * scale)[:heads], (f * scale)[heads:] * lam], axis=0)
        for f in factors
    ]
    gain = gain_ref[...]
    for b in range(rows):
        first = weighted(refs, weights, b, b * vecs, heads, 0)
        second = weighted(refs, weights, b, b * vecs + heads, heads, heads)
        out = first - second
        mean_sq = jnp.mean(out * out, axis=1, keepdims=True)
        n_scr[:, b, :] = out * lax.rsqrt(mean_sq + 1.0 / ctx) * gain
    normed = jnp.concatenate([n_scr[h].astype(BF16) for h in range(heads)], axis=1)
    res = (tok_ref[...].astype(F32) + dot(normed, w_ref[...])).astype(BF16)
    res_ref[...] = res
    for t in range(all_ref.shape[0]):
        all_ref[t] = res
    rest = at + vecs
    a, b_, c, d = [r[rest:].astype(F32) for r in refs]
    kv = (a + b_) + (c + d)
    inv = inv_ref[...]
    for t in range(2):
        nk_ref[:, t, :] = (kv[t * rows : (t + 1) * rows] * inv).astype(BF16)
        nv_ref[:, t, :] = (kv[(2 + t) * rows : (3 + t) * rows] * inv).astype(BF16)


def diagonal(size):
    a = lax.broadcasted_iota(jnp.int32, (size, size), 0)
    return a == lax.broadcasted_iota(jnp.int32, (size, size), 1)


def up_body(res_ref, gain_ref, w_ref, out_ref):
    groups, rows, width = res_ref.shape
    batch = groups * rows
    res = res_ref[...].reshape(batch, width).astype(F32)
    gained = (res * gain_ref[...]).astype(BF16)
    squares = jnp.sum(res * res, axis=1, keepdims=True)
    line = jnp.sum(jnp.where(diagonal(batch), squares, 0.0), axis=0, keepdims=True)
    hi, mid, lo = pieces(jnp.broadcast_to(line, (16, batch)))
    sub = lax.broadcasted_iota(jnp.int32, (16, batch), 0)
    tail = jnp.where(sub == 0, hi, jnp.where(sub == 1, mid, jnp.where(sub == 2, lo, 0.0)))
    tail = tail.astype(BF16)
    up = dot(gained, w_ref[...])
    for d in range(out_ref.shape[0]):
        out_ref[d, :batch] = up[:, d * LANES : (d + 1) * LANES].astype(BF16)
        out_ref[d, batch:] = tail


def act_body(width, in_ref, out_ref):
    peers, batch, _ = out_ref.shape
    up = in_ref[0, :batch].astype(F32)
    tail = in_ref[0, batch:].astype(F32)
    for p in range(1, peers):
        up = up + in_ref[p, :batch].astype(F32)
        tail = tail + in_ref[p, batch:].astype(F32)
    line = jnp.sum(tail, axis=0, keepdims=True)
    squares = jnp.sum(jnp.where(diagonal(batch), line, 0.0), axis=1, keepdims=True)
    pre = up * lax.rsqrt(squares / width + EPS)
    act = jnp.square(jnp.maximum(pre, 0.0)).astype(BF16)
    for p in range(peers):
        out_ref[p] = act


def down_body(act_ref, w_ref, out_ref):
    peers = act_ref.shape[0]
    acts = jnp.concatenate([act_ref[p] for p in range(peers)], axis=1)
    down = dot(acts, w_ref[...]).astype(BF16)
    out_ref[...] = down.reshape(out_ref.shape)


def final_body(down_ref, res_ref, out_ref):
    total = down_ref[0].astype(F32)
    for t in range(1, down_ref.shape[0]):
        total = total + down_ref[t].astype(F32)
    out_ref[...] = (res_ref[...].astype(F32) + total).astype(BF16)


def shards(
    tokens,
    cache_keys,
    cache_values,
    attn_gain,
    w_query,
    w_key,
    w_value,
    lambdas,
    head_gain,
    w_out,
    mlp_gain,
    w_up,
    w_down,
):
    rows, tok_width = tokens.shape
    n_kv = lax.axis_size(KV)
    n_tp = lax.axis_size(TP)
    width = tok_width * n_kv
    heads = lambdas.shape[0]
    ctx_local, kv_heads, _ = cache_keys.shape[1:]
    ctx = ctx_local * n_kv
    spots = ctx_local * kv_heads
    vecs = 2 * heads
    struct = jax.ShapeDtypeStruct
    batch = rows * n_tp

    tok = tokens.astype(F32)
    scaled = (tok * attn_gain[None, :]).astype(BF16)
    squares = jnp.sum(tok * tok, axis=1, keepdims=True)
    q_part = local_call(
        query_body,
        "query",
        struct((heads + 1, rows, LANES), F32),
        scaled,
        jnp.broadcast_to(squares, (rows, LANES)),
        w_query,
        flops=2 * rows * tok_width * w_query.shape[1],
    )
    kv_part = local_call(
        new_kv_body,
        "new_kv",
        struct((4 * rows, LANES), BF16),
        scaled,
        w_key,
        w_value,
        flops=1 << 33,
    )
    a, b, c = from_peers(q_part, "x")
    q_half = (q_part + a) + (b + c)
    a, b, c = from_peers(q_half, "z")
    packed = rows * vecs + vecs + 4 * rows
    payload, inv_one = local_call(
        functools.partial(attention_body, float(width)),
        "attention",
        (struct((packed, LANES), BF16), struct((rows, LANES), F32)),
        q_half,
        a,
        b,
        c,
        kv_part,
        cache_keys.reshape(rows, spots, LANES),
        cache_values.reshape(rows, spots, LANES),
        flops=4 * rows * vecs * spots * LANES,
        limit=24,
        scratch=(
            pltpu.VMEM((rows, heads, LANES), F32),
            pltpu.VMEM((2, vecs, spots), F32),
        ),
    )
    payload = local_call(
        functools.partial(merge_body, rows, vecs),
        "merge",
        struct((packed, LANES), BF16),
        payload,
        *from_peers(payload, "x"),
        flops=packed * LANES * 8,
    )
    residual, to_all, new_keys, new_values = local_call(
        functools.partial(residual_body, rows, vecs, float(ctx)),
        "residual",
        (
            struct((rows, tok_width), BF16),
            struct((n_tp, rows, tok_width), BF16),
            struct((rows, kv_heads, LANES), BF16),
            struct((rows, kv_heads, LANES), BF16),
        ),
        payload,
        *from_peers(payload, "z"),
        inv_one,
        jnp.broadcast_to(lambdas[:, None], (heads, LANES)),
        head_gain[None, :],
        tokens,
        w_out,
        flops=2 * rows * heads * LANES * tok_width,
        scratch=(pltpu.VMEM((heads, rows, LANES), F32),),
    )
    everyone = exchanged(to_all, TP)
    up = local_call(
        up_body,
        "up",
        struct((n_kv, batch + 16, LANES), BF16),
        everyone,
        mlp_gain[None, :],
        w_up,
        flops=2 * batch * tok_width * n_kv * LANES,
    )
    acts = local_call(
        functools.partial(act_body, float(width)),
        "act",
        struct((n_kv, batch, LANES), BF16),
        exchanged(up, KV),
        flops=batch * LANES * 40,
    )
    down = local_call(
        down_body,
        "down",
        struct((n_tp, rows, tok_width), BF16),
        exchanged(acts, KV),
        w_down,
        flops=2 * batch * tok_width * n_kv * LANES,
    )
    mixed = local_call(
        final_body,
        "final",
        struct((rows, tok_width), BF16),
        exchanged(down, TP),
        residual,
        flops=rows * tok_width * 10,
    )
    return mixed, new_keys, new_values


def solution(mesh):
    split = Mesh(mesh.devices.reshape(4, 4, 4, 2), ("z", "x", "y", "c"))
    placed = (
        P(TP, KV),
        P(TP, KV, None, None),
        P(TP, KV, None, None),
        P(KV),
        P(KV, None),
        P(KV, None),
        P(KV, None),
        P(),
        P(),
        P(None, KV),
        P(KV),
        P(KV, TP),
        P(TP, KV),
    )
    return jax.shard_map(
        shards,
        mesh=split,
        in_specs=placed,
        out_specs=(P(TP, KV), P(TP, None, None), P(TP, None, None)),
        check_vma=False,
    )
```

```python
import functools

import jax
import jax.numpy as jnp
from jax import lax
from jax.experimental import pallas as pl
from jax.experimental.pallas import tpu as pltpu
from jax.sharding import Mesh
from jax.sharding import PartitionSpec as P

KV = ("z", "x")
TP = ("y", "c")
EPS = 1e-06
LANES = 128
F32 = jnp.float32
BF16 = jnp.bfloat16
VMEM = pl.BlockSpec(memory_space=pltpu.VMEM)
HBM = pl.BlockSpec(memory_space=pltpu.HBM)


def local_call(body, name, outs, *args, flops=0, scratch=(), limit=8, far=()):
    cost = pl.CostEstimate(
        flops=flops,
        bytes_accessed=sum(a.size * a.dtype.itemsize for a in args),
        transcendentals=0,
    )
    return pl.pallas_call(
        body,
        name=name,
        out_shape=outs,
        in_specs=[HBM if i in far else VMEM for i in range(len(args))],
        out_specs=jax.tree.map(lambda _: VMEM, outs),
        scratch_shapes=list(scratch),
        cost_estimate=cost,
        compiler_params=pltpu.CompilerParams(vmem_limit_bytes=int(limit * 2**20)),
    )(*args)


def from_peers(shard, axis):
    peers = lax.axis_size(axis)
    return [
        lax.ppermute(shard, axis, [(i, i ^ k) for i in range(peers)])
        for k in range(1, peers)
    ]


def exchanged(tiles, axis):
    return lax.all_to_all(tiles, axis, 0, 0, tiled=True)


def dot(a, b, contract=((1,), (0,))):
    return lax.dot_general(a, b, (contract, ((), ())), preferred_element_type=F32)


def pieces(x):
    hi = x.astype(BF16).astype(F32)
    mid = (x - hi).astype(BF16).astype(F32)
    lo = (x - hi - mid).astype(BF16).astype(F32)
    return hi, mid, lo


def query_body(scaled_ref, squares_ref, w_ref, q_ref):
    q = dot(scaled_ref[...], w_ref[...])
    tiles = q_ref.shape[0] - 1
    for h in range(tiles):
        q_ref[h] = q[:, h * LANES : (h + 1) * LANES]
    q_ref[tiles] = squares_ref[...]


def new_kv_body(scaled_ref, wk_ref, wv_ref, kv_ref):
    rows = scaled_ref.shape[0]
    at = 0
    for w in (wk_ref, wv_ref):
        part = dot(scaled_ref[...], w[...]).astype(BF16)
        for t in range(part.shape[1] // LANES):
            kv_ref[at : at + rows] = part[:, t * LANES : (t + 1) * LANES]
            at += rows


def attention_body(width, q0, q1, q2, q3, kv_ref, k_ref, v_ref, out_ref, inv_ref, q_scr, s_scr):
    rows, spots, _ = k_ref.shape
    heads = q0.shape[0] - 1
    total_q = (q0[...] + q1[...]) + (q2[...] + q3[...])
    inv = lax.rsqrt(total_q[heads] / width + EPS)
    inv_ref[...] = inv
    for h in range(heads):
        q_scr[:, h, :] = (total_q[h] * inv).astype(BF16).astype(F32) * 0.125
    vecs = 2 * heads
    lane = lax.broadcasted_iota(jnp.int32, (vecs, LANES), 1)
    row = lax.broadcasted_iota(jnp.int32, (vecs, LANES), 0)
    own_half = (lane // 64) == (row // heads)
    wide_lane = lax.broadcasted_iota(jnp.int32, (vecs, spots), 1)
    wide_row = lax.broadcasted_iota(jnp.int32, (vecs, spots), 0)
    own_head = (wide_lane % 2) == ((wide_row % heads) // (heads // 2))

    def scores(b):
        q16 = q_scr[b]
        both = jnp.concatenate([q16, q16], axis=0)
        q32 = jnp.where(own_half, both, 0.0).astype(BF16)
        return dot(q32, k_ref[b], ((1,), (1,)))

    def finish(b, s, stats):
        s = jnp.where(own_head, s, -1e30)
        top = jnp.max(s, axis=1, keepdims=True)
        e = jnp.exp(s - top)
        total = jnp.sum(e, axis=1, keepdims=True)
        acc = dot(e.astype(BF16), v_ref[b])
        out_ref[pl.ds(pl.multiple_of(b * vecs, vecs), vecs), :] = acc.astype(BF16)
        here = (lane % 16) == b
        return jnp.where(
            here & (lane < 48), top, jnp.where(here & (lane < 96), total, stats)
        )

    deep = 4
    s_scr[0] = scores(0)

    def step(i, stats):
        for u in range(deep):
            b = i * deep + u
            current = s_scr[u % 2]
            following = scores(jnp.minimum(b + 1, rows - 1))
            stats = finish(b, current, stats)
            s_scr[(u + 1) % 2] = following
        return stats

    stats = lax.fori_loop(0, rows // deep, step, jnp.zeros((vecs, LANES), F32))
    hi, mid, lo = pieces(stats)
    kind = (lane // 16) % 3
    at = rows * vecs
    out_ref[at : at + vecs] = jnp.where(
        kind == 0, hi, jnp.where(kind == 1, mid, lo)
    ).astype(BF16)
    out_ref[at + vecs :] = kv_ref[...]


def opened_stats(ref, at, vecs):
    p = ref[at : at + vecs].astype(F32)
    whole = p + pltpu.roll(p, LANES - 16, 1) + pltpu.roll(p, LANES - 32, 1)
    return whole, pltpu.roll(whole, LANES - 48, 1)


def merged_stats(refs, at, vecs):
    opened = [opened_stats(r, at, vecs) for r in refs]
    tops = [o[0] for o in opened]
    peak = jnp.maximum(jnp.maximum(tops[0], tops[1]), jnp.maximum(tops[2], tops[3]))
    factors = [jnp.exp(t - peak) for t in tops]
    parts = [f * o[1] for f, o in zip(factors, opened)]
    total = (parts[0] + parts[1]) + (parts[2] + parts[3])
    return peak, total, factors


def weighted(refs, weights, b, start, count, weight_row):
    parts = []
    for r, w in zip(refs, weights):
        block = r[start : start + count].astype(F32)
        parts.append(block * w[weight_row : weight_row + count, b : b + 1])
    return (parts[0] + parts[1]) + (parts[2] + parts[3])


def merge_body(rows, vecs, p0, p1, p2, p3, out_ref):
    refs = (p0, p1, p2, p3)
    at = rows * vecs
    peak, total, factors = merged_stats(refs, at, vecs)
    for b in range(rows):
        acc = weighted(refs, factors, b, b * vecs, vecs, 0)
        out_ref[b * vecs : (b + 1) * vecs] = acc.astype(BF16)
    lane = lax.broadcasted_iota(jnp.int32, (vecs, LANES), 1)
    both = jnp.where(lane < 16, peak, 0.0)
    both = both + pltpu.roll(both, 16, 1) + pltpu.roll(both, 32, 1)
    tot = jnp.where(lane < 16, total, 0.0)
    tot = pltpu.roll(tot, 48, 1) + pltpu.roll(tot, 64, 1) + pltpu.roll(tot, 80, 1)
    hi, mid, lo = pieces(both + tot)
    kind = (lane // 16) % 3
    out_ref[at : at + vecs] = jnp.where(
        kind == 0, hi, jnp.where(kind == 1, mid, lo)
    ).astype(BF16)
    rest = at + vecs
    a, b_, c, d = [r[rest:].astype(F32) for r in refs]
    out_ref[rest:] = ((a + b_) + (c + d)).astype(BF16)


def residual_body(
    rows, vecs, ctx, p0, p1, p2, p3, lam_ref, gain_ref, tok_ref, w_ref,
    res_ref, all_ref, kv_ref, n_scr,
):
    refs = (p0, p1, p2, p3)
    heads = vecs // 2
    at = rows * vecs
    _, total, factors = merged_stats(refs, at, vecs)
    lane = lax.broadcasted_iota(jnp.int32, (vecs, LANES), 1)
    scale = 1.0 / jnp.where(lane < 16, total, 1.0)
    lam = lam_ref[...]
    weights = [
        jnp.concatenate([(f * scale)[:heads], (f * scale)[heads:] * lam], axis=0)
        for f in factors
    ]
    gain = gain_ref[...]
    for b in range(rows):
        first = weighted(refs, weights, b, b * vecs, heads, 0)
        second = weighted(refs, weights, b, b * vecs + heads, heads, heads)
        out = first - second
        mean_sq = jnp.mean(out * out, axis=1, keepdims=True)
        n_scr[:, b, :] = out * lax.rsqrt(mean_sq + 1.0 / ctx) * gain
    normed = jnp.concatenate([n_scr[h].astype(BF16) for h in range(heads)], axis=1)
    res = (tok_ref[...].astype(F32) + dot(normed, w_ref[...])).astype(BF16)
    res_ref[...] = res
    for t in range(all_ref.shape[0]):
        all_ref[t] = res
    rest = at + vecs
    a, b_, c, d = [r[rest:].astype(F32) for r in refs]
    kv_ref[...] = (a + b_) + (c + d)


def diagonal(size):
    a = lax.broadcasted_iota(jnp.int32, (size, size), 0)
    return a == lax.broadcasted_iota(jnp.int32, (size, size), 1)


def up_body(res_ref, gain_ref, w_ref, out_ref):
    groups, rows, width = res_ref.shape
    batch = groups * rows
    res = res_ref[...].reshape(batch, width).astype(F32)
    gained = (res * gain_ref[...]).astype(BF16)
    squares = jnp.sum(res * res, axis=1, keepdims=True)
    line = jnp.sum(jnp.where(diagonal(batch), squares, 0.0), axis=0, keepdims=True)
    hi, mid, lo = pieces(jnp.broadcast_to(line, (16, batch)))
    sub = lax.broadcasted_iota(jnp.int32, (16, batch), 0)
    tail = jnp.where(sub == 0, hi, jnp.where(sub == 1, mid, jnp.where(sub == 2, lo, 0.0)))
    tail = tail.astype(BF16)
    up = dot(gained, w_ref[...])
    for d in range(out_ref.shape[0]):
        out_ref[d, :batch] = up[:, d * LANES : (d + 1) * LANES].astype(BF16)
        out_ref[d, batch:] = tail


def act_body(width, in_ref, out_ref):
    peers, batch, _ = out_ref.shape
    up = in_ref[0, :batch].astype(F32)
    tail = in_ref[0, batch:].astype(F32)
    for p in range(1, peers):
        up = up + in_ref[p, :batch].astype(F32)
        tail = tail + in_ref[p, batch:].astype(F32)
    line = jnp.sum(tail, axis=0, keepdims=True)
    squares = jnp.sum(jnp.where(diagonal(batch), line, 0.0), axis=1, keepdims=True)
    pre = up * lax.rsqrt(squares / width + EPS)
    act = jnp.square(jnp.maximum(pre, 0.0)).astype(BF16)
    for p in range(peers):
        out_ref[p] = act


def down_body(act_ref, w_ref, out_ref):
    peers = act_ref.shape[0]
    acts = jnp.concatenate([act_ref[p] for p in range(peers)], axis=1)
    down = dot(acts, w_ref[...]).astype(BF16)
    out_ref[...] = down.reshape(out_ref.shape)


def final_body(down_ref, res_ref, kv_ref, inv_ref, out_ref, nk_ref, nv_ref):
    total = down_ref[0].astype(F32)
    for t in range(1, down_ref.shape[0]):
        total = total + down_ref[t].astype(F32)
    out_ref[...] = (res_ref[...].astype(F32) + total).astype(BF16)
    rows = inv_ref.shape[0]
    inv = inv_ref[...]
    for t in range(2):
        nk_ref[:, t, :] = (kv_ref[t * rows : (t + 1) * rows] * inv).astype(BF16)
        nv_ref[:, t, :] = (kv_ref[(2 + t) * rows : (3 + t) * rows] * inv).astype(BF16)


def shards(
    tokens,
    cache_keys,
    cache_values,
    attn_gain,
    w_query,
    w_key,
    w_value,
    lambdas,
    head_gain,
    w_out,
    mlp_gain,
    w_up,
    w_down,
):
    rows, tok_width = tokens.shape
    n_kv = lax.axis_size(KV)
    n_tp = lax.axis_size(TP)
    width = tok_width * n_kv
    heads = lambdas.shape[0]
    ctx_local, kv_heads, _ = cache_keys.shape[1:]
    ctx = ctx_local * n_kv
    spots = ctx_local * kv_heads
    vecs = 2 * heads
    struct = jax.ShapeDtypeStruct
    batch = rows * n_tp

    tok = tokens.astype(F32)
    scaled = (tok * attn_gain[None, :]).astype(BF16)
    squares = jnp.sum(tok * tok, axis=1, keepdims=True)
    q_part = local_call(
        query_body,
        "query",
        struct((heads + 1, rows, LANES), F32),
        scaled,
        jnp.broadcast_to(squares, (rows, LANES)),
        w_query,
        flops=2 * rows * tok_width * w_query.shape[1],
    )
    kv_part = local_call(
        new_kv_body,
        "new_kv",
        struct((4 * rows, LANES), BF16),
        scaled,
        w_key,
        w_value,
        flops=1 << 33,
    )
    a, b, c = from_peers(q_part, "x")
    q_half = (q_part + a) + (b + c)
    a, b, c = from_peers(q_half, "z")
    packed = rows * vecs + vecs + 4 * rows
    payload, inv_one = local_call(
        functools.partial(attention_body, float(width)),
        "attention",
        (struct((packed, LANES), BF16), struct((rows, LANES), F32)),
        q_half,
        a,
        b,
        c,
        kv_part,
        cache_keys.reshape(rows, spots, LANES),
        cache_values.reshape(rows, spots, LANES),
        flops=4 * rows * vecs * spots * LANES,
        limit=24,
        scratch=(
            pltpu.VMEM((rows, heads, LANES), F32),
            pltpu.VMEM((2, vecs, spots), F32),
        ),
    )
    payload = local_call(
        functools.partial(merge_body, rows, vecs),
        "merge",
        struct((packed, LANES), BF16),
        payload,
        *from_peers(payload, "x"),
        flops=packed * LANES * 8,
    )
    residual, to_all, kv_sum = local_call(
        functools.partial(residual_body, rows, vecs, float(ctx)),
        "residual",
        (
            struct((rows, tok_width), BF16),
            struct((n_tp, rows, tok_width), BF16),
            struct((4 * rows, LANES), F32),
        ),
        payload,
        *from_peers(payload, "z"),
        jnp.broadcast_to(lambdas[:, None], (heads, LANES)),
        head_gain[None, :],
        tokens,
        w_out,
        flops=2 * rows * heads * LANES * tok_width,
        scratch=(pltpu.VMEM((heads, rows, LANES), F32),),
    )
    everyone = exchanged(to_all, TP)
    up = local_call(
        up_body,
        "up",
        struct((n_kv, batch + 16, LANES), BF16),
        everyone,
        mlp_gain[None, :],
        w_up,
        flops=2 * batch * tok_width * n_kv * LANES,
    )
    acts = local_call(
        functools.partial(act_body, float(width)),
        "act",
        struct((n_kv, batch, LANES), BF16),
        exchanged(up, KV),
        flops=batch * LANES * 40,
    )
    down = local_call(
        down_body,
        "down",
        struct((n_tp, rows, tok_width), BF16),
        exchanged(acts, KV),
        w_down,
        flops=2 * batch * tok_width * n_kv * LANES,
    )
    mixed, new_keys, new_values = local_call(
        final_body,
        "final",
        (
            struct((rows, tok_width), BF16),
            struct((rows, kv_heads, LANES), BF16),
            struct((rows, kv_heads, LANES), BF16),
        ),
        exchanged(down, TP),
        residual,
        kv_sum,
        inv_one,
        flops=rows * tok_width * 10,
    )
    return mixed, new_keys, new_values


def solution(mesh):
    split = Mesh(mesh.devices.reshape(4, 4, 4, 2), ("z", "x", "y", "c"))
    placed = (
        P(TP, KV),
        P(TP, KV, None, None),
        P(TP, KV, None, None),
        P(KV),
        P(KV, None),
        P(KV, None),
        P(KV, None),
        P(),
        P(),
        P(None, KV),
        P(KV),
        P(KV, TP),
        P(TP, KV),
    )
    return jax.shard_map(
        shards,
        mesh=split,
        in_specs=placed,
        out_specs=(P(TP, KV), P(TP, None, None), P(TP, None, None)),
        check_vma=False,
    )
```

```python
import functools

import jax
import jax.numpy as jnp
from jax import lax
from jax.experimental import pallas as pl
from jax.experimental.pallas import tpu as pltpu
from jax.sharding import Mesh
from jax.sharding import PartitionSpec as P

KV = ("z", "x")
TP = ("y", "c")
EPS = 1e-06
TAIL = 8
LANES = 128
F32 = jnp.float32
BF16 = jnp.bfloat16
VMEM = pl.BlockSpec(memory_space=pltpu.VMEM)
HBM = pl.BlockSpec(memory_space=pltpu.HBM)


def local_call(body, name, outs, *args, flops=0, scratch=(), limit=8, far=()):
    cost = pl.CostEstimate(
        flops=flops,
        bytes_accessed=sum(a.size * a.dtype.itemsize for a in args),
        transcendentals=0,
    )
    return pl.pallas_call(
        body,
        name=name,
        out_shape=outs,
        in_specs=[HBM if i in far else VMEM for i in range(len(args))],
        out_specs=jax.tree.map(lambda _: VMEM, outs),
        scratch_shapes=list(scratch),
        cost_estimate=cost,
        compiler_params=pltpu.CompilerParams(vmem_limit_bytes=int(limit * 2**20)),
    )(*args)


def from_peers(shard, axis):
    peers = lax.axis_size(axis)
    return [
        lax.ppermute(shard, axis, [(i, i ^ k) for i in range(peers)])
        for k in range(1, peers)
    ]


def exchanged(tiles, axis):
    return lax.all_to_all(tiles, axis, 0, 0, tiled=True)


def dot(a, b, contract=((1,), (0,))):
    return lax.dot_general(a, b, (contract, ((), ())), preferred_element_type=F32)


def pieces(x):
    hi = x.astype(BF16).astype(F32)
    mid = (x - hi).astype(BF16).astype(F32)
    lo = (x - hi - mid).astype(BF16).astype(F32)
    return hi, mid, lo


def new_kv_body(scaled_ref, wk_ref, wv_ref, kv_ref):
    at = 0
    for w in (wk_ref, wv_ref):
        part = dot(scaled_ref[...], w[...])
        for t in range(part.shape[1] // LANES):
            kv_ref[at] = part[:, t * LANES : (t + 1) * LANES]
            at += 1


def attention_body(width, q_ref, kv_ref, k_ref, v_ref, out_ref, q_scr, s_scr):
    rows, spots, _ = k_ref.shape
    heads = q_ref.shape[1] // LANES - 1
    inv = lax.rsqrt(q_ref[:, heads * LANES :] * (32.0 / width) + EPS)
    rest = rows * 2 * heads + 2 * heads
    for t in range(kv_ref.shape[0]):
        out_ref[rest + t * rows : rest + (t + 1) * rows] = (kv_ref[t] * inv).astype(BF16)
    for h in range(heads):
        part = q_ref[:, h * LANES : (h + 1) * LANES] * 0.125 * inv
        q_scr[h * rows : (h + 1) * rows] = part.astype(BF16).astype(F32) * 0.125
    vecs = 2 * heads
    lane = lax.broadcasted_iota(jnp.int32, (vecs, LANES), 1)
    row = lax.broadcasted_iota(jnp.int32, (vecs, LANES), 0)
    own_half = (lane // 64) == (row // heads)
    wide_lane = lax.broadcasted_iota(jnp.int32, (vecs, spots), 1)
    wide_row = lax.broadcasted_iota(jnp.int32, (vecs, spots), 0)
    own_head = (wide_lane % 2) == ((wide_row % heads) // (heads // 2))

    def scores(b):
        q16 = q_scr[pl.ds(b, heads, stride=rows), :]
        both = jnp.concatenate([q16, q16], axis=0)
        q32 = jnp.where(own_half, both, 0.0).astype(BF16)
        return dot(q32, k_ref[b], ((1,), (1,)))

    def finish(b, s, stats):
        s = jnp.where(own_head, s, -1e30)
        top = jnp.max(s, axis=1, keepdims=True)
        e = jnp.exp(s - top)
        total = jnp.sum(e, axis=1, keepdims=True)
        acc = dot(e.astype(BF16), v_ref[b])
        out_ref[pl.ds(pl.multiple_of(b * vecs, vecs), vecs), :] = acc.astype(BF16)
        here = (lane % 16) == b
        return jnp.where(
            here & (lane < 48), top, jnp.where(here & (lane < 96), total, stats)
        )

    deep = 16
    s_scr[0] = scores(0)

    def step(i, stats):
        for u in range(deep):
            b = i * deep + u
            current = s_scr[u % 2]
            following = scores(jnp.minimum(b + 1, rows - 1))
            stats = finish(b, current, stats)
            s_scr[(u + 1) % 2] = following
        return stats

    stats = lax.fori_loop(0, rows // deep, step, jnp.zeros((vecs, LANES), F32))
    hi, mid, lo = pieces(stats)
    kind = (lane // 16) % 3
    at = rows * vecs
    out_ref[at : at + vecs] = jnp.where(
        kind == 0, hi, jnp.where(kind == 1, mid, lo)
    ).astype(BF16)


def opened_stats(ref, at, vecs):
    p = ref[at : at + vecs].astype(F32)
    whole = p + pltpu.roll(p, LANES - 16, 1) + pltpu.roll(p, LANES - 32, 1)
    return whole, pltpu.roll(whole, LANES - 48, 1)


def merged_stats(refs, at, vecs):
    opened = [opened_stats(r, at, vecs) for r in refs]
    tops = [o[0] for o in opened]
    peak = jnp.maximum(jnp.maximum(tops[0], tops[1]), jnp.maximum(tops[2], tops[3]))
    factors = [jnp.exp(t - peak) for t in tops]
    parts = [f * o[1] for f, o in zip(factors, opened)]
    total = (parts[0] + parts[1]) + (parts[2] + parts[3])
    return peak, total, factors


def weighted(refs, weights, b, start, count, weight_row):
    parts = []
    for r, w in zip(refs, weights):
        block = r[start : start + count].astype(F32)
        parts.append(block * w[weight_row : weight_row + count, b : b + 1])
    return (parts[0] + parts[1]) + (parts[2] + parts[3])


def merge_body(rows, vecs, p0, p1, p2, p3, out_ref):
    refs = (p0, p1, p2, p3)
    at = rows * vecs
    peak, total, factors = merged_stats(refs, at, vecs)
    for b in range(rows):
        acc = weighted(refs, factors, b, b * vecs, vecs, 0)
        out_ref[b * vecs : (b + 1) * vecs] = acc.astype(BF16)
    lane = lax.broadcasted_iota(jnp.int32, (vecs, LANES), 1)
    both = jnp.where(lane < 16, peak, 0.0)
    both = both + pltpu.roll(both, 16, 1) + pltpu.roll(both, 32, 1)
    tot = jnp.where(lane < 16, total, 0.0)
    tot = pltpu.roll(tot, 48, 1) + pltpu.roll(tot, 64, 1) + pltpu.roll(tot, 80, 1)
    hi, mid, lo = pieces(both + tot)
    kind = (lane // 16) % 3
    out_ref[at : at + vecs] = jnp.where(
        kind == 0, hi, jnp.where(kind == 1, mid, lo)
    ).astype(BF16)

    rest = at + vecs
    a, b_, c, d = [r[rest:].astype(F32) for r in refs]
    out_ref[rest:] = ((a + b_) + (c + d)).astype(BF16)


def residual_body(
    rows, vecs, ctx, p0, p1, p2, p3, lam_ref, gain_ref, tok_ref, w_ref,
    res_ref, kv_ref, n_scr,
):
    refs = (p0, p1, p2, p3)
    heads = vecs // 2
    at = rows * vecs
    _, total, factors = merged_stats(refs, at, vecs)
    lane = lax.broadcasted_iota(jnp.int32, (vecs, LANES), 1)
    scale = 1.0 / jnp.where(lane < 16, total, 1.0)
    lam = lam_ref[...]
    weights = [
        jnp.concatenate([(f * scale)[:heads], (f * scale)[heads:] * lam], axis=0)
        for f in factors
    ]
    gain = gain_ref[...]
    for b in range(rows):
        first = weighted(refs, weights, b, b * vecs, heads, 0)
        second = weighted(refs, weights, b, b * vecs + heads, heads, heads)
        out = first - second
        mean_sq = jnp.mean(out * out, axis=1, keepdims=True)
        normed = out * lax.rsqrt(mean_sq + 1.0 / ctx) * gain
        n_scr[b * heads : (b + 1) * heads] = normed
    normed = jnp.concatenate(
        [n_scr[pl.ds(h, rows, stride=heads), :].astype(BF16) for h in range(heads)],
        axis=1,
    )
    res = (tok_ref[...].astype(F32) + dot(normed, w_ref[...])).astype(BF16)
    res_ref[...] = res
    rest = at + vecs
    a, b_, c, d = [r[rest:].astype(F32) for r in refs]
    kv_ref[...] = (a + b_) + (c + d)


def diagonal(size):
    a = lax.broadcasted_iota(jnp.int32, (size, size), 0)
    return a == lax.broadcasted_iota(jnp.int32, (size, size), 1)


def up_body(r0, r1, r2, r3, gain_ref, w_ref, out_ref):
    cores, rows, width = r0.shape
    batch = 4 * cores * rows
    res = jnp.concatenate(
        [r[t].astype(F32) for r in (r0, r1, r2, r3) for t in range(cores)], axis=0
    )
    gained = (res * gain_ref[...]).astype(BF16)
    squares = jnp.sum(res * res, axis=1, keepdims=True)
    line = jnp.sum(jnp.where(diagonal(batch), squares, 0.0), axis=0, keepdims=True)
    hi, mid, lo = pieces(jnp.broadcast_to(line, (TAIL, batch)))
    sub = lax.broadcasted_iota(jnp.int32, (TAIL, batch), 0)
    tail = jnp.where(sub == 0, hi, jnp.where(sub == 1, mid, jnp.where(sub == 2, lo, 0.0)))
    tail = tail.astype(BF16)
    up = dot(gained, w_ref[...])
    for d in range(out_ref.shape[0]):
        out_ref[d, :batch] = up[:, d * LANES : (d + 1) * LANES].astype(BF16)
        out_ref[d, batch:] = tail


def act_body(width, in_ref, out_ref):
    peers, batch, _ = out_ref.shape
    up = in_ref[0, :batch].astype(F32)
    tail = in_ref[0, batch:].astype(F32)
    for p in range(1, peers):
        up = up + in_ref[p, :batch].astype(F32)
        tail = tail + in_ref[p, batch:].astype(F32)
    line = jnp.sum(tail, axis=0, keepdims=True)
    squares = jnp.sum(jnp.where(diagonal(batch), line, 0.0), axis=1, keepdims=True)
    pre = up * lax.rsqrt(squares / width + EPS)
    act = jnp.square(jnp.maximum(pre, 0.0)).astype(BF16)
    for p in range(peers):
        out_ref[p] = act


def down_body(act_ref, w_ref, *out_refs):
    peers = act_ref.shape[0]
    acts = jnp.concatenate([act_ref[p] for p in range(peers)], axis=1)
    down = dot(acts, w_ref[...]).astype(BF16)
    size = down.shape[0] // len(out_refs)
    for k, out_ref in enumerate(out_refs):
        out_ref[...] = down[k * size : (k + 1) * size].reshape(out_ref.shape)


def sum_body(d0, d1, d2, d3, own_ref, other_ref):
    a, b, c, d = [r[...].astype(F32) for r in (d0, d1, d2, d3)]
    total = (a + b) + (c + d)
    own_ref[...] = total[0]
    other_ref[...] = total[1]


def final_body(own_ref, other_ref, res_ref, kv_ref, out_ref, nk_ref, nv_ref):
    total = own_ref[...] + other_ref[...]
    out_ref[...] = (res_ref[...].astype(F32) + total).astype(BF16)
    rows = out_ref.shape[0]
    for t in range(2):
        nk_ref[:, t, :] = kv_ref[t * rows : (t + 1) * rows].astype(BF16)
        nv_ref[:, t, :] = kv_ref[(2 + t) * rows : (3 + t) * rows].astype(BF16)


def shards(
    tokens,
    cache_keys,
    cache_values,
    attn_gain,
    w_query,
    w_key,
    w_value,
    lambdas,
    head_gain,
    w_out,
    mlp_gain,
    w_up,
    w_down,
):
    rows, tok_width = tokens.shape
    n_kv = lax.axis_size(KV)
    n_tp = lax.axis_size(TP)
    width = tok_width * n_kv
    heads = lambdas.shape[0]
    ctx_local, kv_heads, _ = cache_keys.shape[1:]
    ctx = ctx_local * n_kv
    spots = ctx_local * kv_heads
    vecs = 2 * heads
    struct = jax.ShapeDtypeStruct
    batch = rows * n_tp

    tok = tokens.astype(F32)
    scaled = (tok * attn_gain[None, :]).astype(BF16)
    squares = jnp.sum(tok * tok, axis=1, keepdims=True)
    query = dot(scaled, w_query) * 32.0
    spread = jnp.broadcast_to(squares * 0.125, (rows, LANES))
    q_part = jnp.concatenate([query, spread], axis=1)
    kv_part = local_call(
        new_kv_body,
        "new_kv",
        struct((4, rows, LANES), F32),
        scaled,
        w_key,
        w_value,
        flops=1 << 33,
    )
    q_part = q_part.astype(jnp.float16)
    a, b, c = [p.astype(F32) for p in from_peers(q_part, "z")]
    q_half = (((q_part.astype(F32) + a) + (b + c)) * 0.25).astype(jnp.float16)
    a, b, c = [p.astype(F32) for p in from_peers(q_half, "x")]
    total_q = (q_half.astype(F32) + a) + (b + c)
    packed = rows * vecs + vecs + 4 * rows
    payload = local_call(
        functools.partial(attention_body, float(width)),
        "attention",
        struct((packed, LANES), BF16),
        total_q,
        kv_part,
        cache_keys.reshape(rows, spots, LANES),
        cache_values.reshape(rows, spots, LANES),
        flops=4 * rows * vecs * spots * LANES,
        limit=24,
        scratch=(
            pltpu.VMEM((heads * rows, LANES), F32),
            pltpu.VMEM((2, vecs, spots), F32),
        ),
    )
    payload = local_call(
        functools.partial(merge_body, rows, vecs),
        "merge",
        struct((packed, LANES), BF16),
        payload,
        *from_peers(payload, "x"),
        flops=packed * LANES * 8,
    )
    residual, kv_sum = local_call(
        functools.partial(residual_body, rows, vecs, float(ctx)),
        "residual",
        (
            struct((rows, tok_width), BF16),
            struct((4 * rows, LANES), F32),
        ),
        payload,
        *from_peers(payload, "z"),
        jnp.broadcast_to(lambdas[:, None], (heads, LANES)),
        head_gain[None, :],
        tokens,
        w_out,
        flops=2 * rows * heads * LANES * tok_width,
        scratch=(pltpu.VMEM((rows * heads, LANES), F32),),
    )
    pair = jnp.stack([residual, lax.ppermute(residual, "c", [(0, 1), (1, 0)])])
    everyone = [pair, *from_peers(pair, "y")]
    up = local_call(
        up_body,
        "up",
        struct((n_kv, batch + TAIL, LANES), BF16),
        *everyone,
        mlp_gain[None, :],
        w_up,
        flops=2 * batch * tok_width * n_kv * LANES,
    )
    acts = local_call(
        functools.partial(act_body, float(width)),
        "act",
        struct((n_kv, batch, LANES), BF16),
        exchanged(up, KV),
        flops=batch * LANES * 40,
    )
    down = local_call(
        down_body,
        "down",
        (struct((2, rows, tok_width), BF16),) * 4,
        exchanged(acts, KV),
        w_down,
        flops=2 * batch * tok_width * n_kv * LANES,
    )
    arrived = [
        lax.ppermute(d, "y", [(i, i ^ k) for i in range(4)])
        for k, d in enumerate(down)
        if k
    ]
    own, other = local_call(
        sum_body,
        "sum",
        (struct((rows, tok_width), F32),) * 2,
        down[0],
        *arrived,
        flops=rows * tok_width * 16,
    )
    mixed, new_keys, new_values = local_call(
        final_body,
        "final",
        (
            struct((rows, tok_width), BF16),
            struct((rows, kv_heads, LANES), BF16),
            struct((rows, kv_heads, LANES), BF16),
        ),
        own,
        lax.ppermute(other, "c", [(0, 1), (1, 0)]),
        residual,
        kv_sum,
        flops=rows * tok_width * 10,
    )
    return mixed, new_keys, new_values


def solution(mesh):
    split = Mesh(mesh.devices.reshape(4, 4, 4, 2), ("z", "x", "y", "c"))
    placed = (
        P(TP, KV),
        P(TP, KV, None, None),
        P(TP, KV, None, None),
        P(KV),
        P(KV, None),
        P(KV, None),
        P(KV, None),
        P(),
        P(),
        P(None, KV),
        P(KV),
        P(KV, TP),
        P(TP, KV),
    )
    return jax.shard_map(
        shards,
        mesh=split,
        in_specs=placed,
        out_specs=(P(TP, KV), P(TP, None, None), P(TP, None, None)),
        check_vma=False,
    )
```

```python
import functools

import jax
import jax.numpy as jnp
from jax import lax
from jax.experimental import pallas as pl
from jax.experimental.pallas import tpu as pltpu
from jax.sharding import Mesh
from jax.sharding import PartitionSpec as P

KV = ("z", "x")
TP = ("y", "c")
EPS = 1e-06
TAIL = 8
LANES = 128
F32 = jnp.float32
BF16 = jnp.bfloat16
VMEM = pl.BlockSpec(memory_space=pltpu.VMEM)
HBM = pl.BlockSpec(memory_space=pltpu.HBM)


def local_call(body, name, outs, *args, flops=0, scratch=(), limit=8, far=()):
    cost = pl.CostEstimate(
        flops=flops,
        bytes_accessed=sum(a.size * a.dtype.itemsize for a in args),
        transcendentals=0,
    )
    return pl.pallas_call(
        body,
        name=name,
        out_shape=outs,
        in_specs=[HBM if i in far else VMEM for i in range(len(args))],
        out_specs=jax.tree.map(lambda _: VMEM, outs),
        scratch_shapes=list(scratch),
        cost_estimate=cost,
        compiler_params=pltpu.CompilerParams(vmem_limit_bytes=int(limit * 2**20)),
    )(*args)


def from_peers(shard, axis):
    peers = lax.axis_size(axis)
    return [
        lax.ppermute(shard, axis, [(i, i ^ k) for i in range(peers)])
        for k in range(1, peers)
    ]


def exchanged(tiles, axis):
    return lax.all_to_all(tiles, axis, 0, 0, tiled=True)


def dot(a, b, contract=((1,), (0,))):
    return lax.dot_general(a, b, (contract, ((), ())), preferred_element_type=F32)


def pieces(x):
    hi = x.astype(BF16).astype(F32)
    mid = (x - hi).astype(BF16).astype(F32)
    lo = (x - hi - mid).astype(BF16).astype(F32)
    return hi, mid, lo


def hold_body(in_ref, out_ref):
    out_ref[...] = in_ref[...]


def attention_body(width, q_ref, scaled_ref, wk_ref, wv_ref, k_ref, v_ref, out_ref, q_scr, s_scr):
    rows, spots, _ = k_ref.shape
    heads = q_ref.shape[1] // LANES - 1
    inv = lax.rsqrt(q_ref[:, heads * LANES :] * (32.0 / width) + EPS)
    rest = rows * 2 * heads + 2 * heads
    for w in (wk_ref, wv_ref):
        part = dot(scaled_ref[...], w[...])
        for t in range(part.shape[1] // LANES):
            tile = part[:, t * LANES : (t + 1) * LANES] * inv
            out_ref[rest : rest + rows] = tile.astype(BF16)
            rest += rows
    for h in range(heads):
        part = q_ref[:, h * LANES : (h + 1) * LANES] * 0.125 * inv
        q_scr[h * rows : (h + 1) * rows] = part.astype(BF16).astype(F32) * 0.125
    vecs = 2 * heads
    lane = lax.broadcasted_iota(jnp.int32, (vecs, LANES), 1)
    row = lax.broadcasted_iota(jnp.int32, (vecs, LANES), 0)
    own_half = (lane // 64) == (row // heads)
    wide_lane = lax.broadcasted_iota(jnp.int32, (vecs, spots), 1)
    wide_row = lax.broadcasted_iota(jnp.int32, (vecs, spots), 0)
    own_head = (wide_lane % 2) == ((wide_row % heads) // (heads // 2))

    def scores(b):
        q16 = q_scr[pl.ds(b, heads, stride=rows), :]
        both = jnp.concatenate([q16, q16], axis=0)
        q32 = jnp.where(own_half, both, 0.0).astype(BF16)
        return dot(q32, k_ref[b], ((1,), (1,)))

    def finish(b, s, stats):
        s = jnp.where(own_head, s, -1e30)
        top = jnp.max(s, axis=1, keepdims=True)
        e = jnp.exp(s - top)
        total = jnp.sum(e, axis=1, keepdims=True)
        acc = dot(e.astype(BF16), v_ref[b])
        out_ref[pl.ds(pl.multiple_of(b * vecs, vecs), vecs), :] = acc.astype(BF16)
        here = (lane % 16) == b
        return jnp.where(
            here & (lane < 48), top, jnp.where(here & (lane < 96), total, stats)
        )

    deep = 16
    s_scr[0] = scores(0)

    def step(i, stats):
        for u in range(deep):
            b = i * deep + u
            current = s_scr[u % 2]
            following = scores(jnp.minimum(b + 1, rows - 1))
            stats = finish(b, current, stats)
            s_scr[(u + 1) % 2] = following
        return stats

    stats = lax.fori_loop(0, rows // deep, step, jnp.zeros((vecs, LANES), F32))
    hi, mid, lo = pieces(stats)
    kind = (lane // 16) % 3
    at = rows * vecs
    out_ref[at : at + vecs] = jnp.where(
        kind == 0, hi, jnp.where(kind == 1, mid, lo)
    ).astype(BF16)


def opened_stats(ref, at, vecs):
    p = ref[at : at + vecs].astype(F32)
    whole = p + pltpu.roll(p, LANES - 16, 1) + pltpu.roll(p, LANES - 32, 1)
    return whole, pltpu.roll(whole, LANES - 48, 1)


def merged_stats(refs, at, vecs):
    opened = [opened_stats(r, at, vecs) for r in refs]
    tops = [o[0] for o in opened]
    peak = jnp.maximum(jnp.maximum(tops[0], tops[1]), jnp.maximum(tops[2], tops[3]))
    factors = [jnp.exp(t - peak) for t in tops]
    parts = [f * o[1] for f, o in zip(factors, opened)]
    total = (parts[0] + parts[1]) + (parts[2] + parts[3])
    return peak, total, factors


def weighted(refs, weights, b, start, count, weight_row):
    parts = []
    for r, w in zip(refs, weights):
        block = r[start : start + count].astype(F32)
        parts.append(block * w[weight_row : weight_row + count, b : b + 1])
    return (parts[0] + parts[1]) + (parts[2] + parts[3])


def merge_body(rows, vecs, p0, p1, p2, p3, out_ref):
    refs = (p0, p1, p2, p3)
    at = rows * vecs
    peak, total, factors = merged_stats(refs, at, vecs)
    for b in range(rows):
        acc = weighted(refs, factors, b, b * vecs, vecs, 0)
        out_ref[b * vecs : (b + 1) * vecs] = acc.astype(BF16)
    lane = lax.broadcasted_iota(jnp.int32, (vecs, LANES), 1)
    both = jnp.where(lane < 16, peak, 0.0)
    both = both + pltpu.roll(both, 16, 1) + pltpu.roll(both, 32, 1)
    tot = jnp.where(lane < 16, total, 0.0)
    tot = pltpu.roll(tot, 48, 1) + pltpu.roll(tot, 64, 1) + pltpu.roll(tot, 80, 1)
    hi, mid, lo = pieces(both + tot)
    kind = (lane // 16) % 3
    out_ref[at : at + vecs] = jnp.where(
        kind == 0, hi, jnp.where(kind == 1, mid, lo)
    ).astype(BF16)

    rest = at + vecs
    a, b_, c, d = [r[rest:].astype(F32) for r in refs]
    out_ref[rest:] = ((a + b_) + (c + d)).astype(BF16)


def residual_body(
    rows, vecs, ctx, p0, p1, p2, p3, lam_ref, gain_ref, tok_ref, w_ref,
    res_ref, kv_ref, n_scr,
):
    refs = (p0, p1, p2, p3)
    heads = vecs // 2
    at = rows * vecs
    _, total, factors = merged_stats(refs, at, vecs)
    lane = lax.broadcasted_iota(jnp.int32, (vecs, LANES), 1)
    scale = 1.0 / jnp.where(lane < 16, total, 1.0)
    lam = lam_ref[...]
    weights = [
        jnp.concatenate([(f * scale)[:heads], (f * scale)[heads:] * lam], axis=0)
        for f in factors
    ]
    gain = gain_ref[...]
    for b in range(rows):
        first = weighted(refs, weights, b, b * vecs, heads, 0)
        second = weighted(refs, weights, b, b * vecs + heads, heads, heads)
        out = first - second
        mean_sq = jnp.mean(out * out, axis=1, keepdims=True)
        normed = out * lax.rsqrt(mean_sq + 1.0 / ctx) * gain
        n_scr[b * heads : (b + 1) * heads] = normed
    normed = jnp.concatenate(
        [n_scr[pl.ds(h, rows, stride=heads), :].astype(BF16) for h in range(heads)],
        axis=1,
    )
    res = (tok_ref[...].astype(F32) + dot(normed, w_ref[...])).astype(BF16)
    res_ref[...] = res
    rest = at + vecs
    a, b_, c, d = [r[rest:].astype(F32) for r in refs]
    kv_ref[...] = (a + b_) + (c + d)


def diagonal(size):
    a = lax.broadcasted_iota(jnp.int32, (size, size), 0)
    return a == lax.broadcasted_iota(jnp.int32, (size, size), 1)


def up_body(r0, r1, r2, r3, gain_ref, w_ref, out_ref):
    cores, rows, width = r0.shape
    batch = 4 * cores * rows
    res = jnp.concatenate(
        [r[t].astype(F32) for r in (r0, r1, r2, r3) for t in range(cores)], axis=0
    )
    gained = (res * gain_ref[...]).astype(BF16)
    squares = jnp.sum(res * res, axis=1, keepdims=True)
    line = jnp.sum(jnp.where(diagonal(batch), squares, 0.0), axis=0, keepdims=True)
    hi, mid, lo = pieces(jnp.broadcast_to(line, (TAIL, batch)))
    sub = lax.broadcasted_iota(jnp.int32, (TAIL, batch), 0)
    tail = jnp.where(sub == 0, hi, jnp.where(sub == 1, mid, jnp.where(sub == 2, lo, 0.0)))
    tail = tail.astype(BF16)
    up = dot(gained, w_ref[...])
    for d in range(out_ref.shape[0]):
        out_ref[d, :batch] = up[:, d * LANES : (d + 1) * LANES].astype(BF16)
        out_ref[d, batch:] = tail


def act_body(width, in_ref, out_ref):
    peers, batch, _ = out_ref.shape
    up = in_ref[0, :batch].astype(F32)
    tail = in_ref[0, batch:].astype(F32)
    for p in range(1, peers):
        up = up + in_ref[p, :batch].astype(F32)
        tail = tail + in_ref[p, batch:].astype(F32)
    line = jnp.sum(tail, axis=0, keepdims=True)
    squares = jnp.sum(jnp.where(diagonal(batch), line, 0.0), axis=1, keepdims=True)
    pre = up * lax.rsqrt(squares / width + EPS)
    act = jnp.square(jnp.maximum(pre, 0.0)).astype(BF16)
    for p in range(peers):
        out_ref[p] = act


def down_body(act_ref, w_ref, *out_refs):
    peers = act_ref.shape[0]
    acts = jnp.concatenate([act_ref[p] for p in range(peers)], axis=1)
    down = dot(acts, w_ref[...]).astype(BF16)
    size = down.shape[0] // len(out_refs)
    for k, out_ref in enumerate(out_refs):
        out_ref[...] = down[k * size : (k + 1) * size].reshape(out_ref.shape)


def sum_body(d0, d1, d2, d3, own_ref, other_ref):
    a, b, c, d = [r[...].astype(F32) for r in (d0, d1, d2, d3)]
    total = (a + b) + (c + d)
    own_ref[...] = total[0]
    other_ref[...] = total[1]


def final_body(own_ref, other_ref, res_ref, kv_ref, out_ref, nk_ref, nv_ref):
    total = own_ref[...] + other_ref[...]
    out_ref[...] = (res_ref[...].astype(F32) + total).astype(BF16)
    rows = out_ref.shape[0]
    for t in range(2):
        nk_ref[:, t, :] = kv_ref[t * rows : (t + 1) * rows].astype(BF16)
        nv_ref[:, t, :] = kv_ref[(2 + t) * rows : (3 + t) * rows].astype(BF16)


def shards(
    tokens,
    cache_keys,
    cache_values,
    attn_gain,
    w_query,
    w_key,
    w_value,
    lambdas,
    head_gain,
    w_out,
    mlp_gain,
    w_up,
    w_down,
):
    rows, tok_width = tokens.shape
    n_kv = lax.axis_size(KV)
    n_tp = lax.axis_size(TP)
    width = tok_width * n_kv
    heads = lambdas.shape[0]
    ctx_local, kv_heads, _ = cache_keys.shape[1:]
    ctx = ctx_local * n_kv
    spots = ctx_local * kv_heads
    vecs = 2 * heads
    struct = jax.ShapeDtypeStruct
    batch = rows * n_tp

    tok = tokens.astype(F32)
    scaled = (tok * attn_gain[None, :]).astype(BF16)
    squares = jnp.sum(tok * tok, axis=1, keepdims=True)
    query = dot(scaled, w_query) * 32.0
    spread = jnp.broadcast_to(squares * 0.125, (rows, LANES))
    q_part = jnp.concatenate([query, spread], axis=1)
    held = local_call(
        hold_body,
        "hold",
        struct(scaled.shape, BF16),
        scaled,
        flops=1 << 33,
    )
    q_part = q_part.astype(jnp.float16)
    a, b, c = [p.astype(F32) for p in from_peers(q_part, "z")]
    q_half = (((q_part.astype(F32) + a) + (b + c)) * 0.25).astype(jnp.float16)
    a, b, c = [p.astype(F32) for p in from_peers(q_half, "x")]
    total_q = (q_half.astype(F32) + a) + (b + c)
    packed = rows * vecs + vecs + 4 * rows
    payload = local_call(
        functools.partial(attention_body, float(width)),
        "attention",
        struct((packed, LANES), BF16),
        total_q,
        held,
        w_key,
        w_value,
        cache_keys.reshape(rows, spots, LANES),
        cache_values.reshape(rows, spots, LANES),
        flops=4 * rows * vecs * spots * LANES,
        limit=24,
        scratch=(
            pltpu.VMEM((heads * rows, LANES), F32),
            pltpu.VMEM((2, vecs, spots), F32),
        ),
    )
    payload = local_call(
        functools.partial(merge_body, rows, vecs),
        "merge",
        struct((packed, LANES), BF16),
        payload,
        *from_peers(payload, "x"),
        flops=packed * LANES * 8,
    )
    residual, kv_sum = local_call(
        functools.partial(residual_body, rows, vecs, float(ctx)),
        "residual",
        (
            struct((rows, tok_width), BF16),
            struct((4 * rows, LANES), F32),
        ),
        payload,
        *from_peers(payload, "z"),
        jnp.broadcast_to(lambdas[:, None], (heads, LANES)),
        head_gain[None, :],
        tokens,
        w_out,
        flops=2 * rows * heads * LANES * tok_width,
        scratch=(pltpu.VMEM((rows * heads, LANES), F32),),
    )
    pair = jnp.stack([residual, lax.ppermute(residual, "c", [(0, 1), (1, 0)])])
    everyone = [pair, *from_peers(pair, "y")]
    up = local_call(
        up_body,
        "up",
        struct((n_kv, batch + TAIL, LANES), BF16),
        *everyone,
        mlp_gain[None, :],
        w_up,
        flops=2 * batch * tok_width * n_kv * LANES,
    )
    acts = local_call(
        functools.partial(act_body, float(width)),
        "act",
        struct((n_kv, batch, LANES), BF16),
        exchanged(up, KV),
        flops=batch * LANES * 40,
    )
    down = local_call(
        down_body,
        "down",
        (struct((2, rows, tok_width), BF16),) * 4,
        exchanged(acts, KV),
        w_down,
        flops=2 * batch * tok_width * n_kv * LANES,
    )
    arrived = [
        lax.ppermute(d, "y", [(i, i ^ k) for i in range(4)])
        for k, d in enumerate(down)
        if k
    ]
    own, other = local_call(
        sum_body,
        "sum",
        (struct((rows, tok_width), F32),) * 2,
        down[0],
        *arrived,
        flops=rows * tok_width * 16,
    )
    mixed, new_keys, new_values = local_call(
        final_body,
        "final",
        (
            struct((rows, tok_width), BF16),
            struct((rows, kv_heads, LANES), BF16),
            struct((rows, kv_heads, LANES), BF16),
        ),
        own,
        lax.ppermute(other, "c", [(0, 1), (1, 0)]),
        residual,
        kv_sum,
        flops=rows * tok_width * 10,
    )
    return mixed, new_keys, new_values


def solution(mesh):
    split = Mesh(mesh.devices.reshape(4, 4, 4, 2), ("z", "x", "y", "c"))
    placed = (
        P(TP, KV),
        P(TP, KV, None, None),
        P(TP, KV, None, None),
        P(KV),
        P(KV, None),
        P(KV, None),
        P(KV, None),
        P(),
        P(),
        P(None, KV),
        P(KV),
        P(KV, TP),
        P(TP, KV),
    )
    return jax.shard_map(
        shards,
        mesh=split,
        in_specs=placed,
        out_specs=(P(TP, KV), P(TP, None, None), P(TP, None, None)),
        check_vma=False,
    )
```
